32 devices in a mesh: sp: 8 (over z, y), tp: 4 (over x, core).
Axes of the slice: x: 2, y: 2, z: 4, core: 2. Of those that a mesh axis runs over, the one named last changes fastest.
Arguments:
- layer_input_rows: bfloat16 [2048, 2048], P('sp'), may hold values from -6 to 6
- input_norm_gain: float32 [2048], replicated, may hold values from 0.1 to 1.9
- query_weight: bfloat16 [2048, 1024], P(None, 'tp'), may hold values from -0.125 to 0.125
- key_weight: bfloat16 [2048, 1024], P(None, 'tp'), may hold values from -0.125 to 0.125
- value_weight: bfloat16 [2048, 1024], P(None, 'tp'), may hold values from -0.125 to 0.125
- query_norm_gain: float32 [64], replicated, may hold values from 0.5 to 9
- key_norm_gain: float32 [64], replicated, may hold values from 0.5 to 9
- cumulative_gate: float32 [2048, 16], P('sp', 'tp'), may hold values from -288.72 to 0, as said below
- attention_norm_gain: float32 [1024], P('tp'), may hold values from 0.1 to 1.9
- recurrence_query_weight: bfloat16 [2048, 1024], P(None, 'tp'), may hold values from -0.125 to 0.125
- forget_weight: bfloat16 [2048, 1024], P(None, 'tp'), may hold values from -0.125 to 0.125
- recurrence_value_weight: bfloat16 [2048, 1024], P(None, 'tp'), may hold values from -0.125 to 0.125
- output_gate_weight: bfloat16 [2048, 1024], P(None, 'tp'), may hold values from -0.125 to 0.125
- gate_lower_slack: float32 [1024], P('tp'), may hold values from 0 to 0.06
- extra_log_decay: float32 [2048, 8], P('sp', 'tp'), may hold values from -1.5 to 0
- recurrence_norm_gain: float32 [1024], P('tp'), may hold values from 0.1 to 1.9
- attention_output_weight: bfloat16 [1024, 2048], P('tp'), may hold values from -0.125 to 0.125
- recurrence_output_weight: bfloat16 [1024, 2048], P('tp'), may hold values from -0.125 to 0.125
Outputs:
- mixed: bfloat16 [2048, 2048], P(('sp', 'tp'))
- log_sum: float32 [2048, 16], P('sp', 'tp')
The draws below stay inside these ranges and needn't reach their ends.
Inputs may be any that keep to these rules, and one draw needn't show every extreme that they name: `cumulative_gate`: each column never rises along positions.
All inputs are finite; a program needn't handle non-finite values.
Results may differ from the reference program's by a relative error of at most 0.015.
The reference program's roundings to bfloat16 on the way count: a program that leaves them out, or rounds other values in their place, can miss the bound.
Values may be sent and summed in bfloat16 or wider, within the bound.
A program may use at most 64 MiB of HBM per device.

```python
import math
import jax
import jax.numpy as jnp
from jax import lax

D = 2048
ATT_HEADS = 16
HEAD_DIM = 64
RECURRENCE_HEADS = 8
STATE_ROWS = 128
VAL_DIM = 128
BLOCK = 64
TOKEN_COUNT = 2048
N_TP = 4


def gain_draw(base_key, salt_value):
    subkey = jax.random.fold_in(base_key, salt_value)
    return 1.0 + 0.18 * jax.random.truncated_normal(subkey, -2.5, 2.5, (HEAD_DIM,), jnp.float32)


def draw_query_norm_gain(key, part):
    return gain_draw(key, 11)


def draw_key_norm_gain(key, part):
    return gain_draw(key, 12)


def rough_logs(base_key, head_number, rates):
    random_subkeys = jax.random.split(base_key, 4)
    position_index = jnp.arange(TOKEN_COUNT, dtype=jnp.int32)
    block_of = position_index * 32 // TOKEN_COUNT
    factors = jnp.exp(jax.random.uniform(random_subkeys[0], (32, head_number), jnp.float32, -0.7, 0.7))
    block_scale = jnp.take(factors, block_of, axis=0)
    roughness = jax.random.uniform(random_subkeys[1], (TOKEN_COUNT, head_number), jnp.float32, 0.0, 2.0)
    logit_values = -rates[None, :] * block_scale * roughness
    spike_position = jax.random.randint(random_subkeys[2], (2, head_number), 0, TOKEN_COUNT)
    spike_depth = jnp.log(jax.random.uniform(random_subkeys[3], (2, head_number), jnp.float32, 0.5, 0.8))
    spike_hits = (position_index[:, None, None] == spike_position[None]).astype(jnp.float32)
    return logit_values + jnp.sum(spike_hits * spike_depth[None], axis=1)


def draw_cumulative_gate(key, part):
    random_subkeys = jax.random.split(jax.random.fold_in(key, 21), 4)
    ranking = jax.random.permutation(random_subkeys[0], ATT_HEADS)
    fast_count = ATT_HEADS // 2
    slow_heads = ranking >= fast_count
    slow_rate = jnp.exp(jax.random.uniform(random_subkeys[1], (ATT_HEADS,), jnp.float32, -0.69, 0.69)) / TOKEN_COUNT
    fast_rate = jnp.exp(jax.random.uniform(random_subkeys[2], (ATT_HEADS,), jnp.float32, -4.6, -3.4))
    rates = jnp.where(slow_heads, slow_rate, fast_rate)
    return jnp.cumsum(rough_logs(random_subkeys[3], ATT_HEADS, rates), axis=0)


def draw_extra_log_decay(key, part):
    random_subkeys = jax.random.split(jax.random.fold_in(key, 31), 2)
    rates = jnp.exp(jax.random.uniform(random_subkeys[0], (RECURRENCE_HEADS,), jnp.float32, -2.3, -0.22)) / TOKEN_COUNT
    return rough_logs(random_subkeys[1], RECURRENCE_HEADS, rates)


def draw_gate_lower_slack(key, part):
    random_subkeys = jax.random.split(jax.random.fold_in(key, 41), 3)
    channels = RECURRENCE_HEADS * STATE_ROWS
    ranking = jax.random.permutation(random_subkeys[0], channels)
    fast_count = channels // 2
    slow_rows = ranking >= fast_count
    slow_gap = jnp.exp(jax.random.uniform(random_subkeys[1], (channels,), jnp.float32, -1.6, 0.0)) / TOKEN_COUNT
    fast_gap = jnp.exp(jax.random.uniform(random_subkeys[2], (channels,), jnp.float32, -3.9, -2.82))
    return jnp.where(slow_rows, slow_gap, fast_gap)


def steps_of(rng, shape, cuts, smallest, high):
    loudness = 1.0
    for axis_at, parts in cuts:
        steps = jax.random.uniform(jax.random.fold_in(jax.random.fold_in(rng, 6), axis_at), (parts,), jnp.float32, smallest / len(cuts), high / len(cuts))
        loudness = loudness * jnp.repeat(jnp.exp(steps), shape[axis_at] // parts).reshape((-1,) + (1,) * (len(shape) - 1 - axis_at))
    return loudness


def centred(own_key, extent, spread, limit, pieces=(), kind=jnp.bfloat16):
    level = steps_of(own_key, extent, pieces, -0.22, 0.18) if pieces else 1.0
    array = jax.random.normal(own_key, extent, jnp.float32) * spread * level
    return jnp.minimum(jnp.maximum(array, -limit), limit).astype(kind)


def setup_inputs(seed: int = 0) -> dict:
    arg_keys = jax.random.split(jax.random.key(seed), 19)
    return {
        "layer_input_rows": centred(arg_keys[0], (TOKEN_COUNT, D), 1.0, 6.0, ((0, 8),)),
        "input_norm_gain": jnp.clip(1.0 + 0.18 * jax.random.normal(arg_keys[1], (D,), jnp.float32), 0.1, 1.9),
        "query_weight": centred(arg_keys[2], (D, ATT_HEADS * HEAD_DIM), D ** -0.5, 0.125, ((1, 4),)),
        "key_weight": centred(arg_keys[3], (D, ATT_HEADS * HEAD_DIM), D ** -0.5, 0.125, ((1, 4),)),
        "value_weight": centred(arg_keys[4], (D, ATT_HEADS * HEAD_DIM), D ** -0.5, 0.125, ((1, 4),)),
        "query_norm_gain": draw_query_norm_gain(jax.random.fold_in(arg_keys[18], 71), 0),
        "key_norm_gain": draw_key_norm_gain(jax.random.fold_in(arg_keys[18], 71), 0),
        "cumulative_gate": draw_cumulative_gate(jax.random.fold_in(arg_keys[18], 71), 0),
        "attention_norm_gain": jnp.clip(1.0 + 0.18 * jax.random.normal(arg_keys[8], (ATT_HEADS * HEAD_DIM,), jnp.float32), 0.1, 1.9),
        "recurrence_query_weight": centred(arg_keys[9], (D, RECURRENCE_HEADS * STATE_ROWS), D ** -0.5, 0.125, ((1, 4),)),
        "forget_weight": centred(arg_keys[10], (D, RECURRENCE_HEADS * STATE_ROWS), D ** -0.5, 0.125, ((1, 4),)),
        "recurrence_value_weight": centred(arg_keys[11], (D, RECURRENCE_HEADS * VAL_DIM), D ** -0.5, 0.125, ((1, 4),)),
        "output_gate_weight": centred(arg_keys[12], (D, RECURRENCE_HEADS * VAL_DIM), D ** -0.5, 0.125, ((1, 4),)),
        "gate_lower_slack": draw_gate_lower_slack(jax.random.fold_in(arg_keys[18], 71), 0),
        "extra_log_decay": draw_extra_log_decay(jax.random.fold_in(arg_keys[18], 71), 0),
        "recurrence_norm_gain": jnp.clip(1.0 + 0.18 * jax.random.normal(arg_keys[15], (RECURRENCE_HEADS * VAL_DIM,), jnp.float32), 0.1, 1.9),
        "attention_output_weight": centred(arg_keys[16], (ATT_HEADS * HEAD_DIM, D), (ATT_HEADS * HEAD_DIM + RECURRENCE_HEADS * VAL_DIM) ** -0.5, 0.125, ((0, 4),)),
        "recurrence_output_weight": centred(arg_keys[17], (RECURRENCE_HEADS * VAL_DIM, D), (ATT_HEADS * HEAD_DIM + RECURRENCE_HEADS * VAL_DIM) ** -0.5, 0.125, ((0, 4),)),
    }


EPSILON = 1e-06
HIGHEST_ACCURACY = lax.Precision.HIGHEST

def rms_rows(values, gain):
    squares = lax.optimization_barrier(jnp.mean(values * values, axis=-1, keepdims=True))
    return values * lax.rsqrt(squares + EPSILON) * gain

def recur_blocks(rec_query, forget_fraction, rec_value, decay_logarithm, states):
    length, head_number, keydim = rec_query.shape
    span_rows = BLOCK
    blocks = length // span_rows
    lower_tri = jnp.arange(span_rows)[:, None] >= jnp.arange(span_rows)[None, :]

    def to_blocks(values):
        return values.reshape(blocks, span_rows, head_number, values.shape[-1])

    def advance(carried, inputs):
        current_states, running = carried
        query_block, share_block, value_block, decay_blk = inputs
        within_block = jnp.cumsum(decay_blk, axis=0)
        differ = within_block[:, None] - within_block[None, :]
        fading = jnp.exp(jnp.where(lower_tri[:, :, None, None], differ, -jnp.inf))
        scores = jnp.einsum('thk,tshk,shk->tsh', query_block, fading, share_block, precision=HIGHEST_ACCURACY)
        inner_part = jnp.einsum('tsh,shv->thv', scores, value_block, precision=HIGHEST_ACCURACY)
        carried_piece = jnp.einsum('zbf,bfw->zbw', query_block * jnp.exp(within_block), current_states, precision=HIGHEST_ACCURACY)
        closing_state = within_block[-1]
        current_states = jnp.exp(closing_state)[:, :, None] * current_states + jnp.einsum('tfo,tfw->fow', share_block * jnp.exp(closing_state[None] - within_block), value_block, precision=HIGHEST_ACCURACY)
        visible_query = query_block * jnp.exp(running[None] + within_block)
        return ((current_states, running + closing_state), (inner_part + carried_piece, visible_query))
    zeros_run = jnp.zeros((head_number, keydim), jnp.float32)
    (states, running), (outputs, visible_query) = lax.scan(advance, (states, zeros_run), (to_blocks(rec_query), to_blocks(forget_fraction), to_blocks(rec_value), to_blocks(decay_logarithm)))
    return (outputs.reshape(length, head_number, -1), states, running, visible_query.reshape(length, head_number, keydim))

def attend_head(operands):
    head_query, head_key, head_value, head_cum = operands
    rows_blk = math.gcd(TOKEN_COUNT, 1024)
    score_scale = HEAD_DIM ** (-0.5)
    key_pos = jnp.arange(TOKEN_COUNT, dtype=jnp.int32)

    def one_block(block_index):
        first_row = (block_index * rows_blk).astype(jnp.int32)
        query_block = lax.dynamic_slice_in_dim(head_query, first_row, rows_blk, 0)
        cum_blk = lax.dynamic_slice_in_dim(head_cum, first_row, rows_blk, 0)
        scores = jnp.dot(query_block, head_key.T, preferred_element_type=jnp.float32) * score_scale
        scores = scores + cum_blk[:, None] - head_cum[None, :]
        query_pos = first_row + jnp.arange(rows_blk, dtype=jnp.int32)
        causal = key_pos[None, :] <= query_pos[:, None]
        scores = jnp.where(causal, scores, -jnp.inf)
        row_top = lax.optimization_barrier(jnp.max(scores, axis=-1))
        weights = jnp.exp(scores - row_top[:, None])
        totals = lax.optimization_barrier(jnp.sum(weights, axis=-1))
        summed = jnp.dot(weights.astype(jnp.bfloat16), head_value, preferred_element_type=jnp.float32)
        return (summed / totals[:, None], row_top + jnp.log(totals))
    outputs, log_sums = lax.map(one_block, jnp.arange(TOKEN_COUNT // rows_blk, dtype=jnp.int32))
    return (outputs.reshape(TOKEN_COUNT, HEAD_DIM), log_sums.reshape(TOKEN_COUNT))

def reference(layer_input_rows, input_norm_gain, query_weight, key_weight, value_weight, query_norm_gain, key_norm_gain, cumulative_gate, attention_norm_gain, recurrence_query_weight, forget_weight, recurrence_value_weight, output_gate_weight, gate_lower_slack, extra_log_decay, recurrence_norm_gain, attention_output_weight, recurrence_output_weight):
    normalized_input = rms_rows(layer_input_rows.astype(jnp.float32), input_norm_gain).astype(jnp.bfloat16)

    def project(weight):
        return jnp.dot(normalized_input, weight, preferred_element_type=jnp.float32)
    queries = rms_rows(project(query_weight).reshape(TOKEN_COUNT, ATT_HEADS, HEAD_DIM), query_norm_gain).astype(jnp.bfloat16)
    keys = rms_rows(project(key_weight).reshape(TOKEN_COUNT, ATT_HEADS, HEAD_DIM), key_norm_gain).astype(jnp.bfloat16)
    values = project(value_weight).astype(jnp.bfloat16).reshape(TOKEN_COUNT, ATT_HEADS, HEAD_DIM)
    attention, log_sum = lax.map(attend_head, (queries.transpose(1, 0, 2), keys.transpose(1, 0, 2), values.transpose(1, 0, 2), cumulative_gate.T))
    attn_out = rms_rows(attention.transpose(1, 0, 2), attention_norm_gain.reshape(ATT_HEADS, HEAD_DIM))
    attn_out = attn_out.astype(jnp.bfloat16).reshape(TOKEN_COUNT, ATT_HEADS * HEAD_DIM)
    rec_query = jax.nn.silu(project(recurrence_query_weight)).reshape(TOKEN_COUNT, RECURRENCE_HEADS, STATE_ROWS)
    forget_fraction = gate_lower_slack * jax.nn.sigmoid(-project(forget_weight))
    decay_logarithm = jnp.log1p(-forget_fraction).reshape(TOKEN_COUNT, RECURRENCE_HEADS, STATE_ROWS) + extra_log_decay[:, :, None]
    rec_value = lax.optimization_barrier(project(recurrence_value_weight).astype(jnp.bfloat16)).astype(jnp.float32)
    rec_value = rec_value.reshape(TOKEN_COUNT, RECURRENCE_HEADS, VAL_DIM)
    start_states = jnp.zeros((RECURRENCE_HEADS, STATE_ROWS, VAL_DIM), jnp.float32)
    recurrent_output = recur_blocks(rec_query, forget_fraction.reshape(TOKEN_COUNT, RECURRENCE_HEADS, STATE_ROWS), rec_value, decay_logarithm, start_states)[0]
    out_gate = jax.nn.silu(project(output_gate_weight)).reshape(TOKEN_COUNT, RECURRENCE_HEADS, VAL_DIM)
    rec_out = rms_rows(recurrent_output, recurrence_norm_gain.reshape(RECURRENCE_HEADS, VAL_DIM)) * out_gate
    rec_out = rec_out.astype(jnp.bfloat16).reshape(TOKEN_COUNT, RECURRENCE_HEADS * VAL_DIM)
    attn_cols = ATT_HEADS * HEAD_DIM // N_TP
    rec_cols = RECURRENCE_HEADS * VAL_DIM // N_TP

    def add_group(group_index, running_sum):
        first_attn = (group_index * attn_cols).astype(jnp.int32)
        first_rec = (group_index * rec_cols).astype(jnp.int32)
        attn_part = lax.dynamic_slice_in_dim(attn_out, first_attn, attn_cols, 1)
        attn_rows = lax.dynamic_slice_in_dim(attention_output_weight, first_attn, attn_cols, 0)
        rec_part = lax.dynamic_slice_in_dim(rec_out, first_rec, rec_cols, 1)
        rec_rows = lax.dynamic_slice_in_dim(recurrence_output_weight, first_rec, rec_cols, 0)
        partial_value = jnp.dot(attn_part, attn_rows, preferred_element_type=jnp.float32)
        partial_value = partial_value + jnp.dot(rec_part, rec_rows, preferred_element_type=jnp.float32)
        return running_sum + lax.optimization_barrier(partial_value.astype(jnp.bfloat16)).astype(jnp.float32)
    mixed_sum = lax.fori_loop(0, N_TP, add_group, jnp.zeros((TOKEN_COUNT, D), jnp.float32))
    return (mixed_sum.astype(jnp.bfloat16), log_sum.T)
```

```python
import functools
import math

import jax
import jax.numpy as jnp
from jax import lax
from jax.experimental import pallas as pl
from jax.experimental.pallas import tpu as pltpu
from jax.sharding import PartitionSpec as P

HEAD_DIM = 64
STATE_ROWS = 128
LANES = 128
EPSILON = 1e-06
HIGHEST = lax.Precision.HIGHEST
MESH = pl.DeviceIdType.MESH
F32 = jnp.float32
BF16 = jnp.bfloat16


def dot(a, b):
    return jnp.dot(a, b, preferred_element_type=F32)


def dot_exact(a, b):
    return jnp.dot(a, b, preferred_element_type=F32, precision=HIGHEST)


def dot_nt(a, b, precision=None):
    return lax.dot_general(
        a, b, (((1,), (1,)), ((), ())), preferred_element_type=F32, precision=precision
    )


def iota(shape, axis):
    return lax.broadcasted_iota(jnp.int32, shape, axis)


def grid_of(count):
    columns = max(c for c in range(1, math.isqrt(count) + 1) if count % c == 0)
    return count // columns, columns


def kernel(
    sizes,
    x_hbm, wk_hbm, wv_hbm, wf_hbm, wrv_hbm, wrq_hbm, wq_hbm, wog_hbm, wao_hbm, wro_hbm,
    in_gain, q_gain, k_gain, gate_t, a_gain, slack, extra_t, r_gain,
    mixed_ref, logsum_ref,
    x_v, wk_v, wv_v, wf_v, wrv_v, wrq_v, wq_v, wog_v, wao_v, wro_v,
    xn, kv, gates, q_t, m_s, l_s, acc, attn_t,
    inner, vq, og, ext, st, chain_in, chain_out, incoming, part, mine, send2, recv1, recv2,
    load_sem, col_send, row_send, recv_sem, st_send, st_recv, chain_send, chain_recv,
    s1_send, s1_recv, s2_send, s2_recv,
):
    nz, ny, ntp = sizes
    rows, width = x_v.shape
    cols = wk_v.shape[1]
    heads = cols // HEAD_DIM
    pairs = cols // LANES
    rec_heads = cols // STATE_ROWS
    chips = ntp // 2
    rb = rows // ntp
    pieces = rows // LANES
    stride = rows + pieces * LANES

    sp, tp = lax.axis_index("sp"), lax.axis_index("tp")
    z, y = sp // ny, sp % ny
    chip, core = tp // 2, tp % 2
    partner = chip * 2 + (1 - core)

    loads = []
    for i, (src, dst) in enumerate((
        (x_hbm, x_v), (wk_hbm, wk_v), (wv_hbm, wv_v), (wf_hbm, wf_v), (wrv_hbm, wrv_v),
        (wrq_hbm, wrq_v), (wq_hbm, wq_v), (wog_hbm, wog_v), (wao_hbm, wao_v), (wro_hbm, wro_v),
    )):
        loads.append(pltpu.make_async_copy(src, dst, load_sem.at[i]))
        loads[-1].start()

    barrier = pltpu.get_barrier_semaphore()

    def greet(where):
        pl.semaphore_signal(barrier, inc=1, device_id=where, device_id_type=MESH)

    @pl.when(z > 0)
    def _():
        greet((sp - ny, tp))

    @pl.when(z < nz - 1)
    def _():
        greet((sp + ny, tp))

    for k in range(1, ny):
        greet((z * ny + (y + k) % ny, tp))
    greet((sp, partner))
    for k in range(1, chips):
        greet((sp, ((chip + k) % chips) * 2 + core))

    loads[0].wait()
    xf = x_v[...].astype(F32)
    scale = lax.rsqrt(jnp.mean(xf * xf, axis=-1, keepdims=True) + EPSILON)
    xn[...] = (xf * scale * in_gain[...]).astype(BF16)

    block_ones = jnp.where(
        iota((cols, cols), 0) // HEAD_DIM == iota((cols, cols), 1) // HEAD_DIM, 1.0 / HEAD_DIM, 0.0
    ).astype(F32)
    repeat = (iota((HEAD_DIM, cols), 1) % HEAD_DIM == iota((HEAD_DIM, cols), 0)).astype(F32)

    def head_norm(v, gain_ref):
        mean = dot_exact(v * v, block_ones)
        gain = dot_exact(jnp.broadcast_to(gain_ref[...], (8, HEAD_DIM)), repeat)[0:1]
        return v * lax.rsqrt(mean + EPSILON) * gain

    loads[1].wait()
    keys = head_norm(dot(xn[...], wk_v[...]), k_gain).astype(BF16)
    loads[2].wait()
    values_t = dot(xn[...], wv_v[...]).T.astype(BF16)
    for p in range(pairs):
        lanes = slice(p * LANES, (p + 1) * LANES)
        kv[sp, p * stride : p * stride + rows, :] = keys[:, lanes]
        for i in range(pieces):
            at = p * stride + rows + i * LANES
            kv[sp, at : at + LANES, :] = values_t[lanes, i * LANES : (i + 1) * LANES]
    gates[sp] = jnp.zeros((8, rows), F32)
    gates[sp, 0:heads, :] = gate_t[...]

    def kv_copies(slot, send_sems, where):
        return [
            pltpu.make_async_remote_copy(
                src_ref=buf.at[slot], dst_ref=buf.at[slot], send_sem=send_sems.at[i],
                recv_sem=recv_sem.at[slot, i], device_id=where, device_id_type=MESH,
            )
            for i, buf in enumerate((gates, kv))
        ]

    def up_copies(source_z):
        return kv_copies(source_z * ny + y, col_send.at[source_z], (sp + ny, tp))

    def side_copies(source_z, k):
        return kv_copies(
            source_z * ny + y, row_send.at[source_z, k], (z * ny + (y + k) % ny, tp)
        )

    def wait_block(slot):
        for copy in kv_copies(slot, col_send.at[0], (sp, partner)):
            copy.wait_recv()

    greeted = (ny - 1) + chips + (z > 0).astype(jnp.int32) + (z < nz - 1).astype(jnp.int32)
    pl.semaphore_wait(barrier, greeted)

    @pl.when(z < nz - 1)
    def _():
        for copy in up_copies(z):
            copy.start()

    for k in range(1, ny):
        @pl.when(y + k < ny)
        def _():
            for copy in side_copies(z, k):
                copy.start()

    tri = (iota((rows, rows), 0) >= iota((rows, rows), 1)).astype(F32)
    loads[3].wait()
    share = slack[...] / (1.0 + jnp.exp(dot(xn[...], wf_v[...])))
    run = dot_exact(tri, jnp.log1p(-share))
    ext[...] = jnp.zeros_like(ext)
    ext[0:rec_heads, :] = extra_t[...]
    ext_row = dot_nt(ext[...], tri, HIGHEST)
    ext_col = dot_nt(tri, ext[...], HIGHEST)
    loads[4].wait()
    rec_value = dot(xn[...], wrv_v[...])
    loads[5].wait()
    rec_query = dot(xn[...], wrq_v[...])
    rec_query = rec_query / (1.0 + jnp.exp(-rec_query))
    grown = rec_query * jnp.exp(run)
    last = run[rows - 1 : rows]
    st_rows = STATE_ROWS + 16
    for j in range(rec_heads):
        lanes = slice(j * STATE_ROWS, (j + 1) * STATE_ROWS)
        e_col = ext_col[:, j : j + 1]
        e_row = ext_row[j : j + 1, :]
        e_last = e_row[:, rows - 1 : rows]
        value = rec_value[:, lanes].astype(BF16)
        left = share[:, lanes] * jnp.exp(last[:, lanes] - run[:, lanes] + (e_last - e_col))
        st[y, j * st_rows : j * st_rows + STATE_ROWS, :] = dot(
            rec_value[:, lanes].T.astype(BF16), left.astype(BF16)
        ).astype(BF16)
        st[y, j * st_rows + STATE_ROWS : (j + 1) * st_rows, :] = jnp.broadcast_to(
            jnp.exp(last[:, lanes] + e_last), (16, STATE_ROWS)
        ).astype(BF16)
        scores = dot_nt(
            grown[:, lanes].astype(BF16), (share[:, lanes] * jnp.exp(-run[:, lanes])).astype(BF16)
        )
        fading = jnp.exp(jnp.where(tri > 0.5, e_col - e_row, -jnp.inf))
        scores = jnp.where(tri > 0.5, scores * fading, 0.0)
        inner[:, lanes] = dot(scores.astype(BF16), value)
        vq[:, lanes] = (grown[:, lanes] * jnp.exp(e_col)).astype(BF16)

    def st_copy(k):
        return pltpu.make_async_remote_copy(
            src_ref=st.at[y], dst_ref=st.at[y], send_sem=st_send.at[k], recv_sem=st_recv.at[y],
            device_id=(z * ny + (y + k) % ny, tp), device_id_type=MESH,
        )

    for k in range(1, ny):
        st_copy(k).start()

    loads[6].wait()
    queries_t = (head_norm(dot(xn[...], wq_v[...]), q_gain).astype(BF16).astype(F32)).T
    half_of = iota((LANES, rows), 0) // HEAD_DIM
    for h in range(heads):
        pair = queries_t[(h // 2) * LANES : (h // 2 + 1) * LANES, :] * HEAD_DIM ** (-0.5)
        q_t[h] = jnp.where(half_of == h % 2, pair, 0.0).astype(BF16)

    def attend(slot, own):
        gate = gates[slot].T
        for h in range(heads):
            base = (h // 2) * stride
            s = dot(kv[slot, base : base + rows, :], q_t[h]) - gate[:, h : h + 1]
            if own:
                s = jnp.where(iota((rows, rows), 0) <= iota((rows, rows), 1), s, -jnp.inf)
                top = jnp.max(s, axis=0, keepdims=True)
            else:
                top = jnp.maximum(m_s[h], jnp.max(s, axis=0, keepdims=True))
            weights = jnp.exp(s - top)
            total = jnp.sum(weights, axis=0, keepdims=True)
            at = base + rows + (h % 2) * HEAD_DIM
            v_t = jnp.concatenate(
                [kv[slot, at + i * LANES : at + i * LANES + HEAD_DIM, :] for i in range(pieces)],
                axis=1,
            )
            summed = dot(v_t, weights.astype(BF16))
            if own:
                l_s[h] = total
                acc[h] = summed
            else:
                fade = jnp.exp(m_s[h] - top)
                l_s[h] = l_s[h] * fade + total
                acc[h] = acc[h] * fade + summed
            m_s[h] = top

    attend(sp, True)

    loads[7].wait()
    gate_out = dot(xn[...], wog_v[...])
    og[...] = gate_out / (1.0 + jnp.exp(-gate_out))

    for k in range(1, ny):
        other = (y + k) % ny
        pltpu.make_async_remote_copy(
            src_ref=st.at[other], dst_ref=st.at[other], send_sem=st_send.at[0],
            recv_sem=st_recv.at[other], device_id=(sp, partner), device_id_type=MESH,
        ).wait_recv()

    chain_copy = pltpu.make_async_remote_copy(
        src_ref=chain_out, dst_ref=chain_in, send_sem=chain_send, recv_sem=chain_recv,
        device_id=((sp + ny) % (nz * ny), tp), device_id_type=MESH,
    )

    def advance_chain():
        for j in range(rec_heads):
            rows_at = slice(j * STATE_ROWS, (j + 1) * STATE_ROWS)
            state = chain_in[rows_at, :].astype(F32)
            for k in range(ny):
                @pl.when(y == k)
                def _():
                    incoming[rows_at, :] = state.astype(BF16)

                base = j * st_rows
                decay = st[k, base + STATE_ROWS : base + st_rows, :].astype(F32)[0:1]
                state = state * decay + st[k, base : base + STATE_ROWS, :].astype(F32)
            chain_out[rows_at, :] = state.astype(BF16)

        @pl.when(z < nz - 1)
        def _():
            chain_copy.start()

    @pl.when(z == 0)
    def _():
        chain_in[...] = jnp.zeros_like(chain_in)
        advance_chain()

    for k in range(1, ny):
        @pl.when(y - k >= 0)
        def _():
            wait_block(sp - k)
            attend(sp - k, False)

    def step(d, carry):
        source = z - d
        wait_block(source * ny + y)

        @pl.when(z < nz - 1)
        def _():
            for copy in up_copies(source):
                copy.start()

        for k in range(1, ny):
            for copy in side_copies(source, k):
                copy.start()

        attend(source * ny + y, False)

        @pl.when(d == jnp.maximum(z - 1, 1))
        def _():
            chain_copy.wait_recv()
            advance_chain()

        for k in range(1, ny):
            slot = source * ny + (y + k) % ny
            wait_block(slot)
            attend(slot, False)
        return carry

    lax.fori_loop(1, z + 1, step, 0)

    for h in range(heads):
        mixed = acc[h] / l_s[h]
        mean = jnp.mean(mixed * mixed, axis=0, keepdims=True)
        attn_t[h * HEAD_DIM : (h + 1) * HEAD_DIM, :] = mixed * lax.rsqrt(mean + EPSILON)
        logsum_ref[h : h + 1, :] = m_s[h] + jnp.log(l_s[h]) + gate_t[h : h + 1, :]
    attn_out = (attn_t[...].T * a_gain[...]).astype(BF16)
    for j in range(rec_heads):
        lanes = slice(j * STATE_ROWS, (j + 1) * STATE_ROWS)
        out = inner[:, lanes] + dot_nt(vq[:, lanes], incoming[lanes, :])
        mean = jnp.mean(out * out, axis=-1, keepdims=True)
        out = out * lax.rsqrt(mean + EPSILON) * r_gain[:, lanes] * og[:, lanes]
        vq[:, lanes] = out.astype(BF16)
    loads[8].wait()
    loads[9].wait()
    part[...] = (dot(attn_out, wao_v[...]) + dot(vq[...], wro_v[...])).astype(BF16)

    def rows_of(which_chip, which_core):
        return pl.ds(pl.multiple_of((which_chip * 2 + which_core) * rb, rb), rb)

    def within(j):
        return pltpu.make_async_remote_copy(
            src_ref=part.at[rows_of(j, 1 - core)], dst_ref=recv1.at[j], send_sem=s1_send.at[j],
            recv_sem=s1_recv.at[j], device_id=(sp, partner), device_id_type=MESH,
        )

    def between(j):
        return pltpu.make_async_remote_copy(
            src_ref=send2.at[j], dst_ref=recv2.at[chip], send_sem=s2_send.at[j],
            recv_sem=s2_recv.at[chip], device_id=(sp, j * 2 + core), device_id_type=MESH,
        )

    order = [(chip + k) % chips for k in range(1, chips)] + [chip]
    for j in order:
        within(j).start()
    for j in order[:-1]:
        within(j).wait_recv()
        send2[j] = (part[rows_of(j, core), :].astype(F32) + recv1[j].astype(F32)).astype(BF16)
        between(j).start()
    within(chip).wait_recv()
    mine[...] = part[rows_of(chip, core), :].astype(F32) + recv1[chip].astype(F32)
    for j in order[:-1]:
        pltpu.make_async_remote_copy(
            src_ref=send2.at[j], dst_ref=recv2.at[j], send_sem=s2_send.at[j],
            recv_sem=s2_recv.at[j], device_id=(sp, partner), device_id_type=MESH,
        ).wait_recv()
        mine[...] += recv2[j].astype(F32)
    mixed_ref[...] = mine[...].astype(BF16)

    for j in order:
        within(j).wait_send()
    for j in order[:-1]:
        between(j).wait_send()
    for k in range(1, ny):
        st_copy(k).wait_send()

        @pl.when(y + k < ny)
        def _():
            for copy in side_copies(z, k):
                copy.wait_send()

    @pl.when(z < nz - 1)
    def _():
        chain_copy.wait_send()
        for copy in up_copies(z):
            copy.wait_send()

    def drain(d, carry):
        source = z - d

        @pl.when(z < nz - 1)
        def _():
            for copy in up_copies(source):
                copy.wait_send()

        for k in range(1, ny):
            for copy in side_copies(source, k):
                copy.wait_send()
        return carry

    lax.fori_loop(1, z + 1, drain, 0)


def body(
    n_sp, n_tp,
    layer_input_rows, input_norm_gain, query_weight, key_weight, value_weight, query_norm_gain,
    key_norm_gain, cumulative_gate, attention_norm_gain, recurrence_query_weight, forget_weight,
    recurrence_value_weight, output_gate_weight, gate_lower_slack, extra_log_decay,
    recurrence_norm_gain, attention_output_weight, recurrence_output_weight,
):
    nz, ny = grid_of(n_sp)
    rows, width = layer_input_rows.shape
    cols = query_weight.shape[1]
    heads, pairs, rec_heads = cols // HEAD_DIM, cols // LANES, cols // STATE_ROWS
    rb, chips = rows // n_tp, n_tp // 2
    weight = pltpu.VMEM((width, cols), BF16)
    out_weight = pltpu.VMEM((cols, width), BF16)
    dma = pltpu.SemaphoreType.DMA
    any_space = pl.BlockSpec(memory_space=pl.ANY)
    vmem = pl.BlockSpec(memory_space=pltpu.VMEM)
    mixed, log_sum = pl.pallas_call(
        functools.partial(kernel, (nz, ny, n_tp)),
        name="mixer",
        out_shape=(
            jax.ShapeDtypeStruct((rb, width), BF16),
            jax.ShapeDtypeStruct((heads, rows), F32),
        ),
        in_specs=[any_space] * 10 + [vmem] * 8,
        out_specs=(vmem, vmem),
        scratch_shapes=[
            pltpu.VMEM((rows, width), BF16),
            *([weight] * 7), out_weight, out_weight,
            pltpu.VMEM((rows, width), BF16),
            pltpu.VMEM((n_sp, pairs * 2 * rows, LANES), BF16),
            pltpu.VMEM((n_sp, 8, rows), F32),
            pltpu.VMEM((heads, LANES, rows), BF16),
            pltpu.VMEM((heads, 1, rows), F32),
            pltpu.VMEM((heads, 1, rows), F32),
            pltpu.VMEM((heads, HEAD_DIM, rows), F32),
            pltpu.VMEM((cols, rows), F32),
            pltpu.VMEM((rows, cols), F32),
            pltpu.VMEM((rows, cols), BF16),
            pltpu.VMEM((rows, cols), F32),
            pltpu.VMEM((8, rows), F32),
            pltpu.VMEM((ny, rec_heads * (STATE_ROWS + 16), STATE_ROWS), BF16),
            pltpu.VMEM((cols, STATE_ROWS), BF16),
            pltpu.VMEM((cols, STATE_ROWS), BF16),
            pltpu.VMEM((cols, STATE_ROWS), BF16),
            pltpu.VMEM((rows, width), BF16),
            pltpu.VMEM((rb, width), F32),
            pltpu.VMEM((chips, rb, width), BF16),
            pltpu.VMEM((chips, rb, width), BF16),
            pltpu.VMEM((chips, rb, width), BF16),
            dma((10,)),
            dma((nz, 2)), dma((nz, ny, 2)), dma((n_sp, 2)),
            dma((ny,)), dma((ny,)), dma, dma,
            dma((chips,)), dma((chips,)), dma((chips,)), dma((chips,)),
        ],
        compiler_params=pltpu.CompilerParams(
            collective_id=0, has_side_effects=True, vmem_limit_bytes=60 * 1024 * 1024
        ),
    )(
        layer_input_rows, key_weight, value_weight, forget_weight, recurrence_value_weight,
        recurrence_query_weight, query_weight, output_gate_weight, attention_output_weight,
        recurrence_output_weight,
        input_norm_gain.reshape(1, -1), query_norm_gain.reshape(1, -1),
        key_norm_gain.reshape(1, -1), cumulative_gate.T, attention_norm_gain.reshape(1, -1),
        gate_lower_slack.reshape(1, -1), extra_log_decay.T, recurrence_norm_gain.reshape(1, -1),
    )
    return mixed, log_sum.T


def solution(mesh):
    return jax.shard_map(
        functools.partial(body, mesh.shape["sp"], mesh.shape["tp"]),
        mesh=mesh,
        in_specs=(
            P("sp", None),
            P(),
            P(None, "tp"),
            P(None, "tp"),
            P(None, "tp"),
            P(),
            P(),
            P("sp", "tp"),
            P("tp"),
            P(None, "tp"),
            P(None, "tp"),
            P(None, "tp"),
            P(None, "tp"),
            P("tp"),
            P("sp", "tp"),
            P("tp"),
            P("tp", None),
            P("tp", None),
        ),
        out_specs=(P(("sp", "tp"), None), P("sp", "tp")),
        check_vma=False,
    )
```

```python
import functools
import math

import jax
import jax.numpy as jnp
from jax import lax
from jax.experimental import pallas as pl
from jax.experimental.pallas import tpu as pltpu
from jax.sharding import PartitionSpec as P

HEAD_DIM = 64
STATE_ROWS = 128
LANES = 128
EPSILON = 1e-06
HIGHEST = lax.Precision.HIGHEST
MESH = pl.DeviceIdType.MESH
F32 = jnp.float32
BF16 = jnp.bfloat16


def dot(a, b):
    return jnp.dot(a, b, preferred_element_type=F32)


def dot_exact(a, b):
    return jnp.dot(a, b, preferred_element_type=F32, precision=HIGHEST)


def dot_nt(a, b, precision=None):
    return lax.dot_general(
        a, b, (((1,), (1,)), ((), ())), preferred_element_type=F32, precision=precision
    )


def iota(shape, axis):
    return lax.broadcasted_iota(jnp.int32, shape, axis)


def grid_of(count):
    columns = max(c for c in range(1, math.isqrt(count) + 1) if count % c == 0)
    return count // columns, columns


def kernel(
    sizes,
    x_hbm, wk_hbm, wv_hbm, wf_hbm, wrv_hbm, wrq_hbm, wq_hbm, wog_hbm, wao_hbm, wro_hbm,
    in_gain, q_gain, k_gain, gate_t, a_gain, slack, extra_t, r_gain,
    mixed_ref, logsum_ref,
    x_v, wk_v, wv_v, wf_v, wrv_v, wrq_v, wq_v, wog_v, wao_v, wro_v,
    xn, kv, gates, q_t, m_s, l_s, acc, attn_t,
    inner, vq, og, ext, st, chain_in, chain_out, incoming, part, send2, recv1, recv2,
    load_sem, col_send, row_send, recv_sem, st_send, st_recv, chain_send, chain_recv,
    s1_send, s1_recv, s2_send, s2_recv,
):
    nz, ny, ntp = sizes
    rows, width = x_v.shape
    cols = wk_v.shape[1]
    heads = cols // HEAD_DIM
    pairs = cols // LANES
    rec_heads = cols // STATE_ROWS
    chips = ntp // 2
    rb = rows // ntp
    pieces = rows // LANES
    splits = s1_send.shape[1]
    part_cols = width // splits

    sp, tp = lax.axis_index("sp"), lax.axis_index("tp")
    z, y = sp // ny, sp % ny
    chip, core = tp // 2, tp % 2
    partner = chip * 2 + (1 - core)

    loads = []
    for i, (src, dst) in enumerate((
        (x_hbm, x_v), (wk_hbm, wk_v), (wv_hbm, wv_v), (wf_hbm, wf_v), (wrv_hbm, wrv_v),
        (wrq_hbm, wrq_v), (wq_hbm, wq_v), (wog_hbm, wog_v), (wao_hbm, wao_v), (wro_hbm, wro_v),
    )):
        loads.append(pltpu.make_async_copy(src, dst, load_sem.at[i]))

    for copy in loads[:3]:
        copy.start()

    barrier = pltpu.get_barrier_semaphore()

    def greet(where):
        pl.semaphore_signal(barrier, inc=1, device_id=where, device_id_type=MESH)

    @pl.when(z > 0)
    def _():
        greet((sp - ny, tp))

    @pl.when(z < nz - 1)
    def _():
        greet((sp + ny, tp))

    for k in range(1, ny):
        greet((z * ny + (y + k) % ny, tp))
    greet((sp, partner))
    for k in range(1, chips):
        greet((sp, ((chip + k) % chips) * 2 + core))

    loads[0].wait()
    for copy in loads[3:6]:
        copy.start()
    xf = x_v[...].astype(F32)
    scale = lax.rsqrt(jnp.mean(xf * xf, axis=-1, keepdims=True) + EPSILON)
    xn[...] = (xf * scale * in_gain[...]).astype(BF16)

    block_ones = jnp.where(
        iota((cols, cols), 0) // HEAD_DIM == iota((cols, cols), 1) // HEAD_DIM, 1.0 / HEAD_DIM, 0.0
    ).astype(F32)
    repeat = (iota((HEAD_DIM, cols), 1) % HEAD_DIM == iota((HEAD_DIM, cols), 0)).astype(F32)

    def head_norm(v, gain_ref):
        mean = dot_exact(v * v, block_ones)
        gain = dot_exact(jnp.broadcast_to(gain_ref[...], (8, HEAD_DIM)), repeat)[0:1]
        return v * lax.rsqrt(mean + EPSILON) * gain

    loads[1].wait()
    keys = head_norm(dot(xn[...], wk_v[...]), k_gain).astype(BF16)
    loads[2].wait()
    for copy in loads[6:]:
        copy.start()
    values_t = dot(xn[...], wv_v[...]).T.astype(BF16)
    for p in range(pairs):
        lanes = slice(p * LANES, (p + 1) * LANES)
        kv[sp, 2 * p] = keys[:, lanes]
        for i in range(pieces):
            kv[sp, 2 * p + 1, i * LANES : (i + 1) * LANES, :] = values_t[
                lanes, i * LANES : (i + 1) * LANES
            ]
    gates[sp] = jnp.zeros((8, rows), F32)
    gates[sp, 0:heads, :] = gate_t[...]

    def piece(slot, i):
        return gates.at[slot] if i == 0 else kv.at[slot, i - 1]

    def piece_copy(slot, i, send, where):
        return pltpu.make_async_remote_copy(
            src_ref=piece(slot, i), dst_ref=piece(slot, i), send_sem=send.at[i],
            recv_sem=recv_sem.at[slot, i], device_id=where, device_id_type=MESH,
        )

    every = range(1 + 2 * pairs)

    def pieces_of(p):
        return ((0,) if p == 0 else ()) + (1 + 2 * p, 2 + 2 * p)

    def up_copy(source_z, i):
        return piece_copy(source_z * ny + y, i, col_send.at[source_z], (sp + ny, tp))

    def side_copy(source_z, k, i):
        where = (z * ny + (y + k) % ny, tp)
        return piece_copy(source_z * ny + y, i, row_send.at[source_z, k], where)

    def wait_pieces(slot, which):
        for i in which:
            piece_copy(slot, i, col_send.at[0], (sp, partner)).wait_recv()

    def pass_on(source_z, p):
        for i in pieces_of(p):
            wait_pieces(source_z * ny + y, (i,))

            @pl.when(z < nz - 1)
            def _():
                up_copy(source_z, i).start()

            for k in range(1, ny):
                side_copy(source_z, k, i).start()

    greeted = (ny - 1) + chips + (z > 0).astype(jnp.int32) + (z < nz - 1).astype(jnp.int32)
    pl.semaphore_wait(barrier, greeted)

    @pl.when(z < nz - 1)
    def _():
        for i in every:
            up_copy(z, i).start()

    for k in range(1, ny):
        @pl.when(y + k < ny)
        def _():
            for i in every:
                side_copy(z, k, i).start()

    tri = (iota((rows, rows), 0) >= iota((rows, rows), 1)).astype(F32)
    loads[3].wait()
    share = slack[...] / (1.0 + jnp.exp(dot(xn[...], wf_v[...])))
    run = dot_exact(tri, jnp.log1p(-share))
    ext[...] = jnp.zeros_like(ext)
    ext[0:rec_heads, :] = extra_t[...]
    ext_row = dot_nt(ext[...], tri, HIGHEST)
    ext_col = dot_nt(tri, ext[...], HIGHEST)
    loads[4].wait()
    rec_value = dot(xn[...], wrv_v[...])
    loads[5].wait()
    rec_query = dot(xn[...], wrq_v[...])
    rec_query = rec_query / (1.0 + jnp.exp(-rec_query))
    grown = rec_query * jnp.exp(run)
    last = run[rows - 1 : rows]
    st_rows = STATE_ROWS + 16
    for j in range(rec_heads):
        lanes = slice(j * STATE_ROWS, (j + 1) * STATE_ROWS)
        e_col = ext_col[:, j : j + 1]
        e_row = ext_row[j : j + 1, :]
        e_last = e_row[:, rows - 1 : rows]
        value = rec_value[:, lanes].astype(BF16)
        left = share[:, lanes] * jnp.exp(last[:, lanes] - run[:, lanes] + (e_last - e_col))
        st[y, j * st_rows : j * st_rows + STATE_ROWS, :] = dot(
            rec_value[:, lanes].T.astype(BF16), left.astype(BF16)
        ).astype(BF16)
        st[y, j * st_rows + STATE_ROWS : (j + 1) * st_rows, :] = jnp.broadcast_to(
            jnp.exp(last[:, lanes] + e_last), (16, STATE_ROWS)
        ).astype(BF16)
        scores = dot_nt(
            grown[:, lanes].astype(BF16), (share[:, lanes] * jnp.exp(-run[:, lanes])).astype(BF16)
        )
        fading = jnp.exp(jnp.where(tri > 0.5, e_col - e_row, -jnp.inf))
        scores = jnp.where(tri > 0.5, scores * fading, 0.0)
        inner[:, lanes] = dot(scores.astype(BF16), value)
        vq[:, lanes] = (grown[:, lanes] * jnp.exp(e_col)).astype(BF16)

    def st_copy(k):
        return pltpu.make_async_remote_copy(
            src_ref=st.at[y], dst_ref=st.at[y], send_sem=st_send.at[k], recv_sem=st_recv.at[y],
            device_id=(z * ny + (y + k) % ny, tp), device_id_type=MESH,
        )

    for k in range(1, ny):
        st_copy(k).start()

    @pl.when(z > 0)
    def _():
        for p in range(pairs):
            pass_on(z - 1, p)

    loads[6].wait()
    queries_t = (head_norm(dot(xn[...], wq_v[...]), q_gain).astype(BF16).astype(F32)).T
    half_of = iota((LANES, rows), 0) // HEAD_DIM
    for h in range(heads):
        pair = queries_t[(h // 2) * LANES : (h // 2 + 1) * LANES, :] * HEAD_DIM ** (-0.5)
        q_t[h] = jnp.where(half_of == h % 2, pair, 0.0).astype(BF16)

    def attend(slot, p, own):
        gate = gates[slot].T
        for h in (2 * p, 2 * p + 1):
            s = dot(kv[slot, 2 * p], q_t[h]) - gate[:, h : h + 1]
            if own:
                s = jnp.where(iota((rows, rows), 0) <= iota((rows, rows), 1), s, -jnp.inf)
                top = jnp.max(s, axis=0, keepdims=True)
            else:
                top = jnp.maximum(m_s[h], jnp.max(s, axis=0, keepdims=True))
            weights = jnp.exp(s - top)
            total = jnp.sum(weights, axis=0, keepdims=True)
            v_t = jnp.concatenate(
                [
                    kv[slot, 2 * p + 1, pl.ds(i * LANES + (h % 2) * HEAD_DIM, HEAD_DIM), :]
                    for i in range(pieces)
                ],
                axis=1,
            )
            summed = dot(v_t, weights.astype(BF16))
            if own:
                l_s[h] = total
                acc[h] = summed
            else:
                fade = jnp.exp(m_s[h] - top)
                l_s[h] = l_s[h] * fade + total
                acc[h] = acc[h] * fade + summed
            m_s[h] = top

    for p in range(pairs):
        attend(sp, p, True)

    loads[7].wait()
    gate_out = dot(xn[...], wog_v[...])
    og[...] = gate_out / (1.0 + jnp.exp(-gate_out))

    for k in range(1, ny):
        other = (y + k) % ny
        pltpu.make_async_remote_copy(
            src_ref=st.at[other], dst_ref=st.at[other], send_sem=st_send.at[0],
            recv_sem=st_recv.at[other], device_id=(sp, partner), device_id_type=MESH,
        ).wait_recv()

    chain_copy = pltpu.make_async_remote_copy(
        src_ref=chain_out, dst_ref=chain_in, send_sem=chain_send, recv_sem=chain_recv,
        device_id=((sp + ny) % (nz * ny), tp), device_id_type=MESH,
    )

    def advance_chain():
        for j in range(rec_heads):
            rows_at = slice(j * STATE_ROWS, (j + 1) * STATE_ROWS)
            state = chain_in[rows_at, :].astype(F32)
            for k in range(ny):
                @pl.when(y == k)
                def _():
                    incoming[rows_at, :] = state.astype(BF16)

                base = j * st_rows
                decay = st[k, base + STATE_ROWS : base + st_rows, :].astype(F32)[0:1]
                state = state * decay + st[k, base : base + STATE_ROWS, :].astype(F32)
            chain_out[rows_at, :] = state.astype(BF16)

        @pl.when(z < nz - 1)
        def _():
            chain_copy.start()

    @pl.when(z == 0)
    def _():
        chain_in[...] = jnp.zeros_like(chain_in)
        advance_chain()

    def attend_beside(d):
        for k in range(1, ny):
            other = (y + k) % ny

            @pl.when((d > 0) | (other < y))
            def _():
                slot = (z - d) * ny + other
                for p in range(pairs):
                    wait_pieces(slot, pieces_of(p))
                    attend(slot, p, False)

    def step(d, carry):
        for p in range(pairs):
            @pl.when(d < z)
            def _():
                pass_on(z - d - 1, p)

            attend((z - d) * ny + y, p, False)

        @pl.when(d == jnp.maximum(z - 1, 1))
        def _():
            chain_copy.wait_recv()
            advance_chain()

        attend_beside(d - 1)
        return carry

    lax.fori_loop(1, z + 1, step, 0)
    attend_beside(z)

    for h in range(heads):
        mixed = acc[h] / l_s[h]
        mean = jnp.mean(mixed * mixed, axis=0, keepdims=True)
        attn_t[h * HEAD_DIM : (h + 1) * HEAD_DIM, :] = mixed * lax.rsqrt(mean + EPSILON)
        logsum_ref[h : h + 1, :] = m_s[h] + jnp.log(l_s[h]) + gate_t[h : h + 1, :]
    attn_out = (attn_t[...].T * a_gain[...]).astype(BF16)
    for j in range(rec_heads):
        lanes = slice(j * STATE_ROWS, (j + 1) * STATE_ROWS)
        out = inner[:, lanes] + dot_nt(vq[:, lanes], incoming[lanes, :])
        mean = jnp.mean(out * out, axis=-1, keepdims=True)
        out = out * lax.rsqrt(mean + EPSILON) * r_gain[:, lanes] * og[:, lanes]
        vq[:, lanes] = out.astype(BF16)
    loads[8].wait()
    loads[9].wait()

    def rows_of(which_chip, which_core):
        return pl.ds(pl.multiple_of((which_chip * 2 + which_core) * rb, rb), rb)

    def columns(q):
        return slice(q * part_cols, (q + 1) * part_cols)

    def within(j, q):
        return pltpu.make_async_remote_copy(
            src_ref=part.at[q, rows_of(j, 1 - core)], dst_ref=recv1.at[j, q],
            send_sem=s1_send.at[j, q], recv_sem=s1_recv.at[j, q], device_id=(sp, partner),
            device_id_type=MESH,
        )

    def between(j, q):
        return pltpu.make_async_remote_copy(
            src_ref=send2.at[j, q], dst_ref=recv2.at[chip, q], send_sem=s2_send.at[j, q],
            recv_sem=s2_recv.at[chip, q], device_id=(sp, j * 2 + core), device_id_type=MESH,
        )

    order = [(chip + k) % chips for k in range(1, chips)]

    def chip_sum(j, q):
        within(j, q).wait_recv()
        return part[q, rows_of(j, core), :].astype(F32) + recv1[j, q].astype(F32)

    def send_sums(q):
        for j in order:
            send2[j, q] = chip_sum(j, q).astype(BF16)
            between(j, q).start()

    for q in range(splits):
        part[q] = (
            dot(attn_out, wao_v[:, columns(q)]) + dot(vq[...], wro_v[:, columns(q)])
        ).astype(BF16)
        for j in order:
            within(j, q).start()
        if q > 0:
            send_sums(q - 1)
    send_sums(splits - 1)
    for q in range(splits):
        within(chip, q).start()
    for q in range(splits):
        total = chip_sum(chip, q)
        for j in order:
            pltpu.make_async_remote_copy(
                src_ref=send2.at[j, q], dst_ref=recv2.at[j, q], send_sem=s2_send.at[j, q],
                recv_sem=s2_recv.at[j, q], device_id=(sp, partner), device_id_type=MESH,
            ).wait_recv()
            total = total + recv2[j, q].astype(F32)
        mixed_ref[:, columns(q)] = total.astype(BF16)

    for q in range(splits):
        for j in order + [chip]:
            within(j, q).wait_send()
        for j in order:
            between(j, q).wait_send()
    for k in range(1, ny):
        st_copy(k).wait_send()

        @pl.when(y + k < ny)
        def _():
            for i in every:
                side_copy(z, k, i).wait_send()

    @pl.when(z < nz - 1)
    def _():
        chain_copy.wait_send()
        for i in every:
            up_copy(z, i).wait_send()

    def drain(d, carry):
        source = z - d

        @pl.when(z < nz - 1)
        def _():
            for i in every:
                up_copy(source, i).wait_send()

        for k in range(1, ny):
            for i in every:
                side_copy(source, k, i).wait_send()
        return carry

    lax.fori_loop(1, z + 1, drain, 0)


def body(
    n_sp, n_tp,
    layer_input_rows, input_norm_gain, query_weight, key_weight, value_weight, query_norm_gain,
    key_norm_gain, cumulative_gate, attention_norm_gain, recurrence_query_weight, forget_weight,
    recurrence_value_weight, output_gate_weight, gate_lower_slack, extra_log_decay,
    recurrence_norm_gain, attention_output_weight, recurrence_output_weight,
):
    nz, ny = grid_of(n_sp)
    rows, width = layer_input_rows.shape
    cols = query_weight.shape[1]
    heads, pairs, rec_heads = cols // HEAD_DIM, cols // LANES, cols // STATE_ROWS
    rb, chips = rows // n_tp, n_tp // 2
    kinds, splits = 1 + 2 * pairs, math.gcd(width // LANES, 4)
    weight = pltpu.VMEM((width, cols), BF16)
    out_weight = pltpu.VMEM((cols, width), BF16)
    dma = pltpu.SemaphoreType.DMA
    any_space = pl.BlockSpec(memory_space=pl.ANY)
    vmem = pl.BlockSpec(memory_space=pltpu.VMEM)
    mixed, log_sum = pl.pallas_call(
        functools.partial(kernel, (nz, ny, n_tp)),
        name="mixer",
        out_shape=(
            jax.ShapeDtypeStruct((rb, width), BF16),
            jax.ShapeDtypeStruct((heads, rows), F32),
        ),
        in_specs=[any_space] * 10 + [vmem] * 8,
        out_specs=(vmem, vmem),
        scratch_shapes=[
            pltpu.VMEM((rows, width), BF16),
            *([weight] * 7), out_weight, out_weight,
            pltpu.VMEM((rows, width), BF16),
            pltpu.VMEM((n_sp, 2 * pairs, rows, LANES), BF16),
            pltpu.VMEM((n_sp, 8, rows), F32),
            pltpu.VMEM((heads, LANES, rows), BF16),
            pltpu.VMEM((heads, 1, rows), F32),
            pltpu.VMEM((heads, 1, rows), F32),
            pltpu.VMEM((heads, HEAD_DIM, rows), F32),
            pltpu.VMEM((cols, rows), F32),
            pltpu.VMEM((rows, cols), F32),
            pltpu.VMEM((rows, cols), BF16),
            pltpu.VMEM((rows, cols), F32),
            pltpu.VMEM((8, rows), F32),
            pltpu.VMEM((ny, rec_heads * (STATE_ROWS + 16), STATE_ROWS), BF16),
            pltpu.VMEM((cols, STATE_ROWS), BF16),
            pltpu.VMEM((cols, STATE_ROWS), BF16),
            pltpu.VMEM((cols, STATE_ROWS), BF16),
            pltpu.VMEM((splits, rows, width // splits), BF16),
            *([pltpu.VMEM((chips, splits, rb, width // splits), BF16)] * 3),
            dma((10,)),
            dma((nz, kinds)), dma((nz, ny, kinds)), dma((n_sp, kinds)),
            dma((ny,)), dma((ny,)), dma, dma,
            *([dma((chips, splits))] * 4),
        ],
        compiler_params=pltpu.CompilerParams(
            collective_id=0, has_side_effects=True, vmem_limit_bytes=60 * 1024 * 1024
        ),
    )(
        layer_input_rows, key_weight, value_weight, forget_weight, recurrence_value_weight,
        recurrence_query_weight, query_weight, output_gate_weight, attention_output_weight,
        recurrence_output_weight,
        input_norm_gain.reshape(1, -1), query_norm_gain.reshape(1, -1),
        key_norm_gain.reshape(1, -1), cumulative_gate.T, attention_norm_gain.reshape(1, -1),
        gate_lower_slack.reshape(1, -1), extra_log_decay.T, recurrence_norm_gain.reshape(1, -1),
    )
    return mixed, log_sum.T


def solution(mesh):
    return jax.shard_map(
        functools.partial(body, mesh.shape["sp"], mesh.shape["tp"]),
        mesh=mesh,
        in_specs=(
            P("sp", None),
            P(),
            P(None, "tp"),
            P(None, "tp"),
            P(None, "tp"),
            P(),
            P(),
            P("sp", "tp"),
            P("tp"),
            P(None, "tp"),
            P(None, "tp"),
            P(None, "tp"),
            P(None, "tp"),
            P("tp"),
            P("sp", "tp"),
            P("tp"),
            P("tp", None),
            P("tp", None),
        ),
        out_specs=(P(("sp", "tp"), None), P("sp", "tp")),
        check_vma=False,
    )
```

```python
import functools
import math

import jax
import jax.numpy as jnp
from jax import lax
from jax.experimental import pallas as pl
from jax.experimental.pallas import tpu as pltpu
from jax.sharding import PartitionSpec as P

HEAD_DIM = 64
STATE_ROWS = 128
LANES = 128
EPSILON = 1e-06
HIGHEST = lax.Precision.HIGHEST
MESH = pl.DeviceIdType.MESH
F32 = jnp.float32
BF16 = jnp.bfloat16


def dot(a, b):
    return jnp.dot(a, b, preferred_element_type=F32)


def dot_exact(a, b):
    return jnp.dot(a, b, preferred_element_type=F32, precision=HIGHEST)


def dot_nt(a, b, precision=None):
    return lax.dot_general(
        a, b, (((1,), (1,)), ((), ())), preferred_element_type=F32, precision=precision
    )


def iota(shape, axis):
    return lax.broadcasted_iota(jnp.int32, shape, axis)


def grid_of(count):
    columns = max(c for c in range(1, math.isqrt(count) + 1) if count % c == 0)
    return count // columns, columns


def kernel(
    sizes,
    x_hbm, wk_hbm, wv_hbm, wf_hbm, wrv_hbm, wrq_hbm, wq_hbm, wog_hbm, wao_hbm, wro_hbm,
    in_gain_hbm, q_gain_hbm, k_gain_hbm, gate_t_hbm, a_gain_hbm,
    slack_hbm, extra_t_hbm, r_gain_hbm,
    mixed_ref, logsum_ref,
    x_v, wk_v, wv_v, wf_v, wrv_v, wrq_v, wq_v, wog_v, wao_v, wro_v,
    xn, kv, gates, q_t, m_s, l_s, acc, attn_t,
    inner, vq, og, ext, st, chain_in, chain_out, incoming, part, send2, recv1, recv2,
    in_gain, q_gain, k_gain, gate_t, a_gain, slack, extra_t, r_gain, rec_part,
    load_sem, col_send, row_send, recv_sem, st_send, st_recv, chain_send, chain_recv,
    s1_send, s1_recv, s2_send, s2_recv,
):
    nz, ny, ntp = sizes
    rows, width = x_v.shape
    cols = wk_v.shape[1]
    heads = cols // HEAD_DIM
    pairs = cols // LANES
    rec_heads = cols // STATE_ROWS
    chips = ntp // 2
    rb = rows // ntp
    pieces = rows // LANES
    splits = s1_send.shape[1]
    part_cols = width // splits

    sp, tp = lax.axis_index("sp"), lax.axis_index("tp")
    z, y = sp // ny, sp % ny
    chip, core = tp // 2, tp % 2
    partner = chip * 2 + (1 - core)

    loads = []
    for i, (src, dst) in enumerate((
        (x_hbm, x_v), (wk_hbm, wk_v), (wv_hbm, wv_v), (wf_hbm, wf_v), (wrv_hbm, wrv_v),
        (wrq_hbm, wrq_v), (wq_hbm, wq_v), (wog_hbm, wog_v), (wao_hbm, wao_v), (wro_hbm, wro_v),
        (in_gain_hbm, in_gain), (q_gain_hbm, q_gain), (k_gain_hbm, k_gain),
        (gate_t_hbm, gate_t), (a_gain_hbm, a_gain), (slack_hbm, slack),
        (extra_t_hbm, extra_t), (r_gain_hbm, r_gain),
    )):
        loads.append(pltpu.make_async_copy(src, dst, load_sem.at[i]))

    for copy in loads[:3] + loads[10:]:
        copy.start()

    barrier = pltpu.get_barrier_semaphore()

    def greet(where):
        pl.semaphore_signal(barrier, inc=1, device_id=where, device_id_type=MESH)

    @pl.when(z > 0)
    def _():
        greet((sp - ny, tp))

    @pl.when(z < nz - 1)
    def _():
        greet((sp + ny, tp))

    for k in range(1, ny):
        greet((z * ny + (y + k) % ny, tp))
    greet((sp, partner))
    for k in range(1, chips):
        greet((sp, ((chip + k) % chips) * 2 + core))

    loads[0].wait()
    for copy in loads[10:]:
        copy.wait()
    for copy in loads[3:6]:
        copy.start()
    xf = x_v[...].astype(F32)
    scale = lax.rsqrt(jnp.mean(xf * xf, axis=-1, keepdims=True) + EPSILON)
    xn[...] = (xf * scale * in_gain[...]).astype(BF16)

    block_ones = jnp.where(
        iota((cols, cols), 0) // HEAD_DIM == iota((cols, cols), 1) // HEAD_DIM, 1.0 / HEAD_DIM, 0.0
    ).astype(F32)
    repeat = (iota((HEAD_DIM, cols), 1) % HEAD_DIM == iota((HEAD_DIM, cols), 0)).astype(F32)

    def head_norm(v, gain_ref):
        mean = dot_exact(v * v, block_ones)
        gain = dot_exact(jnp.broadcast_to(gain_ref[...], (8, HEAD_DIM)), repeat)[0:1]
        return v * lax.rsqrt(mean + EPSILON) * gain

    loads[1].wait()
    keys = head_norm(dot(xn[...], wk_v[...]), k_gain).astype(BF16)
    for p in range(pairs):
        kv[sp, 2 * p] = keys[:, p * LANES : (p + 1) * LANES]
    gates[sp] = jnp.zeros((8, rows), F32)
    gates[sp, 0:heads, :] = gate_t[...]

    def piece(slot, i):
        return gates.at[slot] if i == 0 else kv.at[slot, i - 1]

    def piece_copy(slot, i, send, where):
        return pltpu.make_async_remote_copy(
            src_ref=piece(slot, i), dst_ref=piece(slot, i), send_sem=send.at[i],
            recv_sem=recv_sem.at[slot, i], device_id=where, device_id_type=MESH,
        )

    every = range(1 + 2 * pairs)

    def pieces_of(p):
        return ((0,) if p == 0 else ()) + (1 + 2 * p, 2 + 2 * p)

    def up_copy(source_z, i):
        return piece_copy(source_z * ny + y, i, col_send.at[source_z], (sp + ny, tp))

    def side_copy(source_z, k, i):
        where = (z * ny + (y + k) % ny, tp)
        return piece_copy(source_z * ny + y, i, row_send.at[source_z, k], where)

    def wait_pieces(slot, which):
        for i in which:
            piece_copy(slot, i, col_send.at[0], (sp, partner)).wait_recv()

    def pass_on(source_z, p):
        for i in pieces_of(p):
            wait_pieces(source_z * ny + y, (i,))

            @pl.when(z < nz - 1)
            def _():
                up_copy(source_z, i).start()

            for k in range(1, ny):
                side_copy(source_z, k, i).start()

    greeted = (ny - 1) + chips + (z > 0).astype(jnp.int32) + (z < nz - 1).astype(jnp.int32)
    pl.semaphore_wait(barrier, greeted)

    def start_own(which):
        @pl.when(z < nz - 1)
        def _():
            for i in which:
                up_copy(z, i).start()

        for k in range(1, ny):
            @pl.when(y + k < ny)
            def _():
                for i in which:
                    side_copy(z, k, i).start()

    start_own([0] + [1 + 2 * p for p in range(pairs)])

    loads[2].wait()
    for copy in loads[6:10]:
        copy.start()
    values_t = dot(xn[...], wv_v[...]).T.astype(BF16)
    for p in range(pairs):
        for i in range(pieces):
            kv[sp, 2 * p + 1, i * LANES : (i + 1) * LANES, :] = values_t[
                p * LANES : (p + 1) * LANES, i * LANES : (i + 1) * LANES
            ]
    start_own([2 + 2 * p for p in range(pairs)])

    tri = (iota((rows, rows), 0) >= iota((rows, rows), 1)).astype(F32)
    loads[3].wait()
    share = slack[...] / (1.0 + jnp.exp(dot(xn[...], wf_v[...])))
    run = dot_exact(tri, jnp.log1p(-share))
    ext[...] = jnp.zeros_like(ext)
    ext[0:rec_heads, :] = extra_t[...]
    ext_row = dot_nt(ext[...], tri, HIGHEST)
    ext_col = dot_nt(tri, ext[...], HIGHEST)
    loads[4].wait()
    rec_value = dot(xn[...], wrv_v[...])
    loads[5].wait()
    rec_query = dot(xn[...], wrq_v[...])
    rec_query = rec_query / (1.0 + jnp.exp(-rec_query))
    grown = rec_query * jnp.exp(run)
    last = run[rows - 1 : rows]
    st_rows = STATE_ROWS + 16
    for j in range(rec_heads):
        lanes = slice(j * STATE_ROWS, (j + 1) * STATE_ROWS)
        e_col = ext_col[:, j : j + 1]
        e_row = ext_row[j : j + 1, :]
        e_last = e_row[:, rows - 1 : rows]
        value = rec_value[:, lanes].astype(BF16)
        left = share[:, lanes] * jnp.exp(last[:, lanes] - run[:, lanes] + (e_last - e_col))
        st[y, j * st_rows : j * st_rows + STATE_ROWS, :] = dot(
            rec_value[:, lanes].T.astype(BF16), left.astype(BF16)
        ).astype(BF16)
        st[y, j * st_rows + STATE_ROWS : (j + 1) * st_rows, :] = jnp.broadcast_to(
            jnp.exp(last[:, lanes] + e_last), (16, STATE_ROWS)
        ).astype(BF16)
        scores = dot_nt(
            grown[:, lanes].astype(BF16), (share[:, lanes] * jnp.exp(-run[:, lanes])).astype(BF16)
        )
        fading = jnp.exp(jnp.where(tri > 0.5, e_col - e_row, -jnp.inf))
        scores = jnp.where(tri > 0.5, scores * fading, 0.0)
        inner[:, lanes] = dot(scores.astype(BF16), value)
        vq[:, lanes] = (grown[:, lanes] * jnp.exp(e_col)).astype(BF16)

    def st_copy(k):
        return pltpu.make_async_remote_copy(
            src_ref=st.at[y], dst_ref=st.at[y], send_sem=st_send.at[k], recv_sem=st_recv.at[y],
            device_id=(z * ny + (y + k) % ny, tp), device_id_type=MESH,
        )

    for k in range(1, ny):
        st_copy(k).start()

    @pl.when(z > 0)
    def _():
        for p in range(pairs):
            pass_on(z - 1, p)

    loads[6].wait()
    queries_t = (head_norm(dot(xn[...], wq_v[...]), q_gain).astype(BF16).astype(F32)).T
    half_of = iota((LANES, rows), 0) // HEAD_DIM
    for h in range(heads):
        pair = queries_t[(h // 2) * LANES : (h // 2 + 1) * LANES, :] * HEAD_DIM ** (-0.5)
        q_t[h] = jnp.where(half_of == h % 2, pair, 0.0).astype(BF16)

    def attend(slot, p, own):
        gate = gates[slot].T
        for h in (2 * p, 2 * p + 1):
            s = dot(kv[slot, 2 * p], q_t[h]) - gate[:, h : h + 1]
            if own:
                s = jnp.where(iota((rows, rows), 0) <= iota((rows, rows), 1), s, -jnp.inf)
                top = jnp.max(s, axis=0, keepdims=True)
            else:
                top = jnp.maximum(m_s[h], jnp.max(s, axis=0, keepdims=True))
            weights = jnp.exp(s - top)
            total = jnp.sum(weights, axis=0, keepdims=True)
            v_t = jnp.concatenate(
                [
                    kv[slot, 2 * p + 1, pl.ds(i * LANES + (h % 2) * HEAD_DIM, HEAD_DIM), :]
                    for i in range(pieces)
                ],
                axis=1,
            )
            summed = dot(v_t, weights.astype(BF16))
            if own:
                l_s[h] = total
                acc[h] = summed
            else:
                fade = jnp.exp(m_s[h] - top)
                l_s[h] = l_s[h] * fade + total
                acc[h] = acc[h] * fade + summed
            m_s[h] = top

    for p in range(pairs):
        attend(sp, p, True)

    loads[7].wait()
    gate_out = dot(xn[...], wog_v[...])
    og[...] = gate_out / (1.0 + jnp.exp(-gate_out))

    for k in range(1, ny):
        other = (y + k) % ny
        pltpu.make_async_remote_copy(
            src_ref=st.at[other], dst_ref=st.at[other], send_sem=st_send.at[0],
            recv_sem=st_recv.at[other], device_id=(sp, partner), device_id_type=MESH,
        ).wait_recv()

    chain_copy = pltpu.make_async_remote_copy(
        src_ref=chain_out, dst_ref=chain_in, send_sem=chain_send, recv_sem=chain_recv,
        device_id=((sp + ny) % (nz * ny), tp), device_id_type=MESH,
    )

    def advance_chain():
        for j in range(rec_heads):
            rows_at = slice(j * STATE_ROWS, (j + 1) * STATE_ROWS)
            state = chain_in[rows_at, :].astype(F32)
            for k in range(ny):
                @pl.when(y == k)
                def _():
                    incoming[rows_at, :] = state.astype(BF16)

                base = j * st_rows
                decay = st[k, base + STATE_ROWS : base + st_rows, :].astype(F32)[0:1]
                state = state * decay + st[k, base : base + STATE_ROWS, :].astype(F32)
            chain_out[rows_at, :] = state.astype(BF16)

        @pl.when(z < nz - 1)
        def _():
            chain_copy.start()

    @pl.when(z == 0)
    def _():
        chain_in[...] = jnp.zeros_like(chain_in)
        advance_chain()

    def attend_beside(d):
        for k in range(1, ny):
            other = (y + k) % ny

            @pl.when((d > 0) | (other < y))
            def _():
                slot = (z - d) * ny + other
                for p in range(pairs):
                    wait_pieces(slot, pieces_of(p))
                    attend(slot, p, False)

    def step(d, carry):
        for p in range(pairs):
            @pl.when(d < z)
            def _():
                pass_on(z - d - 1, p)

            attend((z - d) * ny + y, p, False)

        @pl.when(d == jnp.maximum(z - 1, 1))
        def _():
            chain_copy.wait_recv()
            advance_chain()

        attend_beside(d - 1)
        return carry

    lax.fori_loop(1, z + 1, step, 0)
    for j in range(rec_heads):
        lanes = slice(j * STATE_ROWS, (j + 1) * STATE_ROWS)
        out = inner[:, lanes] + dot_nt(vq[:, lanes], incoming[lanes, :])
        mean = jnp.mean(out * out, axis=-1, keepdims=True)
        out = out * lax.rsqrt(mean + EPSILON) * r_gain[:, lanes] * og[:, lanes]
        vq[:, lanes] = out.astype(BF16)
    loads[9].wait()
    rec_part[...] = dot(vq[...], wro_v[...])

    attend_beside(z)

    for h in range(heads):
        mixed = acc[h] / l_s[h]
        mean = jnp.mean(mixed * mixed, axis=0, keepdims=True)
        attn_t[h * HEAD_DIM : (h + 1) * HEAD_DIM, :] = mixed * lax.rsqrt(mean + EPSILON)
        logsum_ref[h : h + 1, :] = m_s[h] + jnp.log(l_s[h]) + gate_t[h : h + 1, :]
    attn_out = (attn_t[...].T * a_gain[...]).astype(BF16)
    loads[8].wait()

    def rows_of(which_chip, which_core):
        return pl.ds(pl.multiple_of((which_chip * 2 + which_core) * rb, rb), rb)

    def columns(q):
        return slice(q * part_cols, (q + 1) * part_cols)

    def within(j, q):
        return pltpu.make_async_remote_copy(
            src_ref=part.at[q, rows_of(j, 1 - core)], dst_ref=recv1.at[j, q],
            send_sem=s1_send.at[j, q], recv_sem=s1_recv.at[j, q], device_id=(sp, partner),
            device_id_type=MESH,
        )

    def between(j, q):
        return pltpu.make_async_remote_copy(
            src_ref=send2.at[j, q], dst_ref=recv2.at[chip, q], send_sem=s2_send.at[j, q],
            recv_sem=s2_recv.at[chip, q], device_id=(sp, j * 2 + core), device_id_type=MESH,
        )

    order = [(chip + k) % chips for k in range(1, chips)]

    def chip_sum(j, q):
        within(j, q).wait_recv()
        return part[q, rows_of(j, core), :].astype(F32) + recv1[j, q].astype(F32)

    def send_sums(q):
        for j in order:
            send2[j, q] = chip_sum(j, q).astype(BF16)
            between(j, q).start()

    for q in range(splits):
        part[q] = (
            dot(attn_out, wao_v[:, columns(q)]) + rec_part[:, columns(q)]
        ).astype(BF16)
        for j in order:
            within(j, q).start()
        if q > 0:
            send_sums(q - 1)
    send_sums(splits - 1)
    for q in range(splits):
        within(chip, q).start()
    for q in range(splits):
        total = chip_sum(chip, q)
        for j in order:
            pltpu.make_async_remote_copy(
                src_ref=send2.at[j, q], dst_ref=recv2.at[j, q], send_sem=s2_send.at[j, q],
                recv_sem=s2_recv.at[j, q], device_id=(sp, partner), device_id_type=MESH,
            ).wait_recv()
            total = total + recv2[j, q].astype(F32)
        mixed_ref[:, columns(q)] = total.astype(BF16)

    for q in range(splits):
        for j in order + [chip]:
            within(j, q).wait_send()
        for j in order:
            between(j, q).wait_send()
    for k in range(1, ny):
        st_copy(k).wait_send()

        @pl.when(y + k < ny)
        def _():
            for i in every:
                side_copy(z, k, i).wait_send()

    @pl.when(z < nz - 1)
    def _():
        chain_copy.wait_send()
        for i in every:
            up_copy(z, i).wait_send()

    def drain(d, carry):
        source = z - d

        @pl.when(z < nz - 1)
        def _():
            for i in every:
                up_copy(source, i).wait_send()

        for k in range(1, ny):
            for i in every:
                side_copy(source, k, i).wait_send()
        return carry

    lax.fori_loop(1, z + 1, drain, 0)


def body(
    n_sp, n_tp,
    layer_input_rows, input_norm_gain, query_weight, key_weight, value_weight, query_norm_gain,
    key_norm_gain, cumulative_gate, attention_norm_gain, recurrence_query_weight, forget_weight,
    recurrence_value_weight, output_gate_weight, gate_lower_slack, extra_log_decay,
    recurrence_norm_gain, attention_output_weight, recurrence_output_weight,
):
    nz, ny = grid_of(n_sp)
    rows, width = layer_input_rows.shape
    cols = query_weight.shape[1]
    heads, pairs, rec_heads = cols // HEAD_DIM, cols // LANES, cols // STATE_ROWS
    rb, chips = rows // n_tp, n_tp // 2
    kinds, splits = 1 + 2 * pairs, math.gcd(width // LANES, 4)
    weight = pltpu.VMEM((width, cols), BF16)
    out_weight = pltpu.VMEM((cols, width), BF16)
    dma = pltpu.SemaphoreType.DMA
    any_space = pl.BlockSpec(memory_space=pl.ANY)
    vmem = pl.BlockSpec(memory_space=pltpu.VMEM)
    mixed, log_sum = pl.pallas_call(
        functools.partial(kernel, (nz, ny, n_tp)),
        name="mixer",
        out_shape=(
            jax.ShapeDtypeStruct((rb, width), BF16),
            jax.ShapeDtypeStruct((heads, rows), F32),
        ),
        in_specs=[any_space] * 18,
        out_specs=(vmem, vmem),
        scratch_shapes=[
            pltpu.VMEM((rows, width), BF16),
            *([weight] * 7), out_weight, out_weight,
            pltpu.VMEM((rows, width), BF16),
            pltpu.VMEM((n_sp, 2 * pairs, rows, LANES), BF16),
            pltpu.VMEM((n_sp, 8, rows), F32),
            pltpu.VMEM((heads, LANES, rows), BF16),
            pltpu.VMEM((heads, 1, rows), F32),
            pltpu.VMEM((heads, 1, rows), F32),
            pltpu.VMEM((heads, HEAD_DIM, rows), F32),
            pltpu.VMEM((cols, rows), F32),
            pltpu.VMEM((rows, cols), F32),
            pltpu.VMEM((rows, cols), BF16),
            pltpu.VMEM((rows, cols), F32),
            pltpu.VMEM((8, rows), F32),
            pltpu.VMEM((ny, rec_heads * (STATE_ROWS + 16), STATE_ROWS), BF16),
            pltpu.VMEM((cols, STATE_ROWS), BF16),
            pltpu.VMEM((cols, STATE_ROWS), BF16),
            pltpu.VMEM((cols, STATE_ROWS), BF16),
            pltpu.VMEM((splits, rows, width // splits), BF16),
            *([pltpu.VMEM((chips, splits, rb, width // splits), BF16)] * 3),
            *([pltpu.VMEM((1, n), F32) for n in (width, HEAD_DIM, HEAD_DIM)]),
            pltpu.VMEM((heads, rows), F32),
            pltpu.VMEM((1, cols), F32),
            pltpu.VMEM((1, cols), F32),
            pltpu.VMEM((rec_heads, rows), F32),
            pltpu.VMEM((1, cols), F32),
            pltpu.VMEM((rows, width), F32),
            dma((18,)),
            dma((nz, kinds)), dma((nz, ny, kinds)), dma((n_sp, kinds)),
            dma((ny,)), dma((ny,)), dma, dma,
            *([dma((chips, splits))] * 4),
        ],
        compiler_params=pltpu.CompilerParams(
            collective_id=0, has_side_effects=True, vmem_limit_bytes=60 * 1024 * 1024
        ),
    )(
        layer_input_rows, key_weight, value_weight, forget_weight, recurrence_value_weight,
        recurrence_query_weight, query_weight, output_gate_weight, attention_output_weight,
        recurrence_output_weight,
        input_norm_gain.reshape(1, -1), query_norm_gain.reshape(1, -1),
        key_norm_gain.reshape(1, -1), cumulative_gate.T, attention_norm_gain.reshape(1, -1),
        gate_lower_slack.reshape(1, -1), extra_log_decay.T, recurrence_norm_gain.reshape(1, -1),
    )
    return mixed, log_sum.T


def solution(mesh):
    return jax.shard_map(
        functools.partial(body, mesh.shape["sp"], mesh.shape["tp"]),
        mesh=mesh,
        in_specs=(
            P("sp", None),
            P(),
            P(None, "tp"),
            P(None, "tp"),
            P(None, "tp"),
            P(),
            P(),
            P("sp", "tp"),
            P("tp"),
            P(None, "tp"),
            P(None, "tp"),
            P(None, "tp"),
            P(None, "tp"),
            P("tp"),
            P("sp", "tp"),
            P("tp"),
            P("tp", None),
            P("tp", None),
        ),
        out_specs=(P(("sp", "tp"), None), P("sp", "tp")),
        check_vma=False,
    )
```
